256 devices in a mesh: grp: 2 (over y), fs: 16 (over z), tp: 8 (over x, core).
Axes of the slice: x: 4, y: 2, z: 16, core: 2. Of those that a mesh axis runs over, the one named last changes fastest.
The devices are a block of a 4x16x16 slice.
Arguments:
- tokens: bfloat16 [32768, 2048], P(('grp', 'fs', 'tp')), parts along dimension 0, may hold values from -12 to 12
- norm_gain: float32 [2048], replicated, may hold values from 0.1 to 1.9
- w_in: bfloat16 [2048, 8192], P('fs', 'tp'), may hold values from -0.125 to 0.125
- w_out: bfloat16 [8192, 2048], P('tp', 'fs'), may hold values from -0.0625 to 0.0625
Outputs:
- mixed: bfloat16 [32768, 2048], P(('grp', 'fs', 'tp')), parts along dimension 0
The draws below stay inside these ranges and needn't reach their ends.
There are 2 independent parts, one for each index of `grp`. The reference program is written for one: setup_inputs(seed, part) draws one part's arguments, and reference() takes and returns one part's arrays. A program takes and returns all parts, laid end to end along the dimension named above; an argument that names none is the same for every part. Nothing has to cross between parts.
All inputs are finite; a program needn't handle non-finite values.
Results may differ from the reference program's by a relative error of at most 0.012.
Values may be sent and summed in bfloat16 or wider, within the bound.
No kernel may reach another device: no remote copies, remote signals or barrier semaphores. Data moves between devices by JAX's collectives and lax.ppermute only.
A program may use at most 64 MiB of HBM per device.

```python
import math
import jax
import jax.numpy as jnp
from jax import lax

D = 2048
FF = 8192
FF_DEV = 1024
TOKENS = 16384
N_TP = 8


def draw_tokens(key, part):
    first = jax.random.fold_in(key, 11)
    second = jax.random.fold_in(key, 12)
    scales = jnp.exp(jax.random.uniform(second, (TOKENS, 1), jnp.float32, math.log(0.35), math.log(2.8)))
    base = jax.random.normal(first, (TOKENS, D), jnp.float32)
    return jnp.clip(base * scales, -12.0, 12.0).astype(jnp.bfloat16)


def block_scale(stream_key, extent, cuts, low, top_value):
    gain, own = 1.0, jax.random.fold_in(stream_key, 6)
    for position, shards_of in cuts:
        steps = jnp.exp(jax.random.uniform(jax.random.fold_in(own, position), (shards_of,), jnp.float32, low / len(cuts), top_value / len(cuts)))
        gain = gain * jnp.repeat(steps, extent[position] // shards_of).reshape([-1 if axis == position else 1 for axis in range(len(extent))])
    return gain


def gaussian(rng, dims, spread, bound, cuts=(), dtype=jnp.bfloat16):
    entries = jax.random.normal(rng, dims, jnp.float32) * spread
    if len(cuts) > 0:
        entries = block_scale(rng, dims, cuts, -0.22, 0.18) * entries
    return jnp.clip(entries, min=-bound, max=bound).astype(dtype)


def setup_inputs(seed: int = 0, part: int = 0) -> dict:
    key_list = jax.random.split(jax.random.key(seed), 5)
    own_keys = jax.random.split(jax.random.fold_in(key_list[4], part), 5)
    tokens = draw_tokens(jax.random.fold_in(jax.random.fold_in(key_list[4], part), 71), part)
    norm_gain = jnp.clip(1.0 + 0.18 * jax.random.normal(key_list[1], (D,), jnp.float32), 0.1, 1.9)
    w_in = gaussian(key_list[2], (D, FF), D ** -0.5, 0.125, ((0, 16), (1, 8)))
    w_out = gaussian(key_list[3], (FF, D), FF ** -0.5, 0.0625, ((0, 8), (1, 16)))
    return dict(tokens=tokens, norm_gain=norm_gain, w_in=w_in, w_out=w_out)


EPS = 1e-06

def reference(tokens, norm_gain, w_in, w_out):
    block = math.gcd(TOKENS, 2048)
    pieces = tokens.reshape(TOKENS // block, block, D)

    def one_block(rows_in):
        xf = rows_in.astype(jnp.float32)
        scale = lax.rsqrt(lax.optimization_barrier(jnp.mean(xf * xf, axis=-1, keepdims=True)) + EPS)
        normed = (xf * scale * norm_gain.astype(jnp.float32)).astype(jnp.bfloat16)
        pre = jnp.dot(normed, w_in, preferred_element_type=jnp.float32)
        hidden = jnp.square(jax.nn.relu(pre)).astype(jnp.bfloat16)
        total = xf
        for index in range(N_TP):
            lower = index * FF_DEV
            partial_sum = jnp.dot(hidden[:, lower:lower + FF_DEV], w_out[lower:lower + FF_DEV, :], preferred_element_type=jnp.float32).astype(jnp.bfloat16)
            partial_sum = lax.optimization_barrier(partial_sum)
            total = total + partial_sum.astype(jnp.float32)
        return total.astype(jnp.bfloat16)
    mixed = lax.map(one_block, pieces)
    return mixed.reshape(TOKENS, D)
```

```python
import functools

import jax
import jax.numpy as jnp
from jax import lax
from jax.experimental import pallas as pl
from jax.experimental.pallas import tpu as pltpu
from jax.sharding import PartitionSpec as P

EPS = 1e-06
CORES = 2
VMEM = pl.BlockSpec(memory_space=pltpu.VMEM)


def call(body, name, out_shape, args, flops):
    size = sum(a.size * a.dtype.itemsize for a in [*args, *jax.tree.leaves(out_shape)])
    return pl.pallas_call(
        body,
        name=name,
        out_shape=out_shape,
        in_specs=[VMEM] * len(args),
        out_specs=jax.tree.map(lambda _: VMEM, out_shape),
        cost_estimate=pl.CostEstimate(flops=flops, bytes_accessed=size, transcendentals=0),
    )(*args)


def block_cols(z, sign, k, n_fs, width):
    b = lax.rem(z + sign * k + n_fs, n_fs)
    return pl.ds(pl.multiple_of(b * width, width), width)


def position():
    sign = 2 * lax.rem(lax.axis_index("tp"), CORES) - 1
    return lax.axis_index("fs"), sign


def norm_body(n_fs, tok_ref, gain_ref, own_ref, par_ref):
    z, sign = position()
    rows, d = tok_ref.shape
    w = d // n_fs
    xf = tok_ref[...].astype(jnp.float32)
    scale = lax.rsqrt(jnp.mean(xf * xf, axis=-1, keepdims=True) + EPS)
    for k in range(n_fs // 2 + 1):
        for ref, s in ((own_ref, sign), (par_ref, -sign)):
            cols = block_cols(z, s, k, n_fs, w)
            part = tok_ref[:, cols].astype(jnp.float32) * scale * gain_ref[:, cols]
            ref[:, k * w : (k + 1) * w] = part.astype(jnp.bfloat16)


def dot1_body(n_a, n_b, tile, x_ref, *refs):
    a_refs, b_refs, out_ref = refs[:n_a], refs[n_a : n_a + n_b], refs[-1]
    f = a_refs[0].shape[1]
    kb = sum(r.shape[0] for r in b_refs)
    skip = a_refs[0].shape[0] * 2

    def step(i, _):
        cols = pl.ds(pl.multiple_of(i * tile, tile), tile)
        wa = jnp.concatenate([r[:, cols] for r in a_refs], axis=0)
        pa = jnp.dot(x_ref[...], wa, preferred_element_type=jnp.float32)
        out_ref[:, cols] = pa.astype(jnp.bfloat16)
        wb = jnp.concatenate([r[:, cols] for r in b_refs], axis=0)
        pb = jnp.dot(x_ref[:, skip : skip + kb], wb, preferred_element_type=jnp.float32)
        out_ref[:, pl.ds(pl.multiple_of(f + i * tile, tile), tile)] = pb.astype(jnp.bfloat16)
        return 0

    lax.fori_loop(0, f // tile, step, 0)


def hidden_body(p_ref, q_ref, h_ref):
    rows, cols = p_ref.shape
    r, f = rows // 2, cols // 2
    for i in range(2):
        for j in range(2):
            pre = p_ref[i * r : (i + 1) * r, j * f : (j + 1) * f].astype(jnp.float32) + q_ref[
                (1 - i) * r : (2 - i) * r, (1 - j) * f : (2 - j) * f
            ].astype(jnp.float32)
            h_ref[i * r : (i + 1) * r, j * f : (j + 1) * f] = jnp.square(jnp.maximum(pre, 0.0)).astype(jnp.bfloat16)


def dot2_body(n_chunks, counts, *refs):
    h_refs, outs = refs[:n_chunks], refs[-n_chunks:]
    w_refs = refs[n_chunks:-n_chunks]
    for h_ref, o_ref in zip(h_refs, outs):
        pos, col = 0, 0
        while pos < len(w_refs):
            here = counts[col]
            blk = w_refs[pos : pos + here]
            pos += here
            w = jnp.concatenate([r[...] for r in blk], axis=0)
            depth = w.shape[0]
            o = jnp.dot(h_ref[:, :depth], w, preferred_element_type=jnp.float32)
            width = w.shape[1]
            o_ref[:, col * width : (col + 1) * width] = o.astype(jnp.bfloat16)
            col += 1


def sum_body(a_ref, b_ref, c_ref, d_ref, s_ref, u_ref):
    r = a_ref.shape[0] // 2
    tot = a_ref[...].astype(jnp.float32) + b_ref[...].astype(jnp.float32)
    tot = tot + (c_ref[...].astype(jnp.float32) + d_ref[...].astype(jnp.float32))
    s_ref[...] = tot[:r]
    u_ref[...] = tot[r:].astype(jnp.bfloat16)


def final_body(n_fs, groups, tok_ref, *refs):
    z, sign = position()
    n = len(groups)
    s_refs, u_refs, out_ref = refs[:n], refs[n : 2 * n], refs[-1]
    w = tok_ref.shape[1] // n_fs
    half = n_fs // 2
    for s_ref, u_ref, ks in zip(s_refs, u_refs, groups):
        for i, k in enumerate(ks):
            here = slice(i * w, (i + 1) * w)
            s, u = s_ref[:, here], u_ref[:, here].astype(jnp.float32)
            cols = block_cols(z, sign, k, n_fs, w)
            if k in (0, half):
                out_ref[:, cols] = (tok_ref[:, cols].astype(jnp.float32) + (s + u)).astype(jnp.bfloat16)
            else:
                out_ref[:, cols] = (tok_ref[:, cols].astype(jnp.float32) + s).astype(jnp.bfloat16)
                cols = block_cols(z, -sign, k, n_fs, w)
                out_ref[:, cols] = (tok_ref[:, cols].astype(jnp.float32) + u).astype(jnp.bfloat16)


def after(x, *deps):
    return lax.optimization_barrier((x, *deps))[0]


def local(n_fs, n_tp, tokens, norm_gain, w_in, w_out):
    half, n_x = n_fs // 2, n_tp // CORES
    axes = ("fs", "tp")
    every = [(f, t) for f in range(n_fs) for t in range(n_tp)]

    def moved(dest):
        flat = lambda f, t: (f % n_fs) * n_tp + t
        return [(flat(f, t), flat(*dest(f, t))) for f, t in every]

    ring = moved(lambda f, t: (f + 1 - 2 * (t % CORES), t))
    swap = moved(lambda f, t: (f, t ^ 1))
    along = [moved(lambda f, t, d=d: (f, (t + CORES * d) % n_tp)) for d in range(n_x)]
    pz = lambda v: lax.ppermute(v, axes, ring)
    pc = lambda v: lax.ppermute(v, axes, swap)
    px = lambda v, d: lax.ppermute(v, axes, along[d % n_x])

    rows, d_model = tokens.shape
    width = d_model // n_fs
    f_own = w_in.shape[1]

    shape = jax.ShapeDtypeStruct((rows, (half + 1) * width), jnp.bfloat16)
    own, par = call(
        functools.partial(norm_body, n_fs),
        "norm",
        (shape, shape),
        (tokens, norm_gain.astype(jnp.float32).reshape(1, d_model)),
        rows * d_model * 8,
    )
    chip = jnp.concatenate([own, pc(par)], axis=0)

    def halves(v):
        h = v.shape[0] // 2
        return [v[:h], v[h:]]

    in_a, in_b = [halves(w_in)], [[pc(v) for v in halves(w_in)]]
    out_a, out_b = [halves(w_out)], [[pc(v) for v in halves(w_out)]]
    for k in range(1, half + 1):
        in_a.append([pz(v) for v in in_a[-1]])
        if k < half:
            in_b.append([pz(v) for v in in_b[-1]])
    gate = in_a[half - 1][0]
    for k in range(1, half + 1):
        if k == 1:
            out_a.append([pz(after(v, gate)) for v in out_a[-1]])
            out_b.append([pz(after(v, gate)) for v in out_b[-1]])
            continue
        out_a.append([pz(v) for v in out_a[-1]])
        if k < half:
            out_b.append([pz(v) for v in out_b[-1]])

    chunks = [chip] + [px(chip, d) for d in range(1, n_x)]
    a_all = [v for blk in in_a for v in blk]
    b_all = [v for blk in in_b[1:half] for v in blk]
    hidden = []
    for x in chunks:
        p = call(
            functools.partial(dot1_body, len(a_all), len(b_all), 256),
            "dot1",
            jax.ShapeDtypeStruct((x.shape[0], CORES * f_own), jnp.bfloat16),
            (x, *a_all, *b_all),
            2 * x.shape[0] * d_model * f_own,
        )
        hidden.append(call(hidden_body, "hidden", jax.ShapeDtypeStruct(p.shape, jnp.bfloat16), (p, pc(p)), p.size * 4))

    groups = [(0, 1, 2), (3, 4), (5, 6), tuple(range(7, half + 1))]
    sums, sides = [], []
    for ks in groups:
        blocks, counts = [], []
        for k in ks:
            blk = out_a[k] + (out_b[k] if 0 < k < half else [])
            blocks += blk
            counts.append(len(blk))
        o_shape = jax.ShapeDtypeStruct((CORES * rows, len(ks) * width), jnp.bfloat16)
        parts = call(
            functools.partial(dot2_body, n_x, tuple(counts)),
            "dot2",
            (o_shape,) * n_x,
            (*hidden, *blocks),
            2 * n_x * CORES * rows * CORES * f_own * len(ks) * width,
        )
        got = [parts[0]] + [px(parts[d], -d) for d in range(1, n_x)]
        s, u = call(
            sum_body,
            "sum",
            (
                jax.ShapeDtypeStruct((rows, len(ks) * width), jnp.float32),
                jax.ShapeDtypeStruct((rows, len(ks) * width), jnp.bfloat16),
            ),
            got,
            4 * o_shape.size,
        )
        sums.append(s)
        sides.append(pc(u))
    return call(
        functools.partial(final_body, n_fs, groups),
        "final",
        jax.ShapeDtypeStruct(tokens.shape, jnp.bfloat16),
        (tokens, *sums, *sides),
        rows * d_model * 4,
    )


def solution(mesh):
    in_specs = (P(("grp", "fs", "tp"), None), P(), P("fs", "tp"), P("tp", "fs"))
    out_specs = P(("grp", "fs", "tp"), None)
    body = functools.partial(local, mesh.shape["fs"], mesh.shape["tp"])
    return jax.shard_map(body, mesh=mesh, in_specs=in_specs, out_specs=out_specs, check_vma=False)
```

```python
import functools

import jax
import jax.numpy as jnp
from jax import lax
from jax.experimental import pallas as pl
from jax.experimental.pallas import tpu as pltpu
from jax.sharding import PartitionSpec as P

EPS = 1e-06
CORES = 2
VMEM = pl.BlockSpec(memory_space=pltpu.VMEM)
SCRATCH = 8 << 20


def call(body, name, out_shape, args, flops):
    size = sum(a.size * a.dtype.itemsize for a in [*args, *jax.tree.leaves(out_shape)])
    return pl.pallas_call(
        body,
        name=name,
        out_shape=jax.tree.map(lambda o: pltpu.VMEM(o.shape, o.dtype), out_shape),
        in_specs=[VMEM] * len(args),
        out_specs=jax.tree.map(lambda _: VMEM, out_shape),
        cost_estimate=pl.CostEstimate(flops=flops, bytes_accessed=size, transcendentals=0),
        compiler_params=pltpu.CompilerParams(vmem_limit_bytes=SCRATCH),
    )(*[pltpu.with_memory_space_constraint(a, pltpu.VMEM) for a in args])


def block_cols(z, sign, k, n_fs, width):
    b = lax.rem(z + sign * k + n_fs, n_fs)
    return pl.ds(pl.multiple_of(b * width, width), width)


def position():
    sign = 2 * lax.rem(lax.axis_index("tp"), CORES) - 1
    return lax.axis_index("fs"), sign


def norm_body(n_fs, tok_ref, gain_ref, own_ref, par_ref):
    z, sign = position()
    rows, d = tok_ref.shape
    w = d // n_fs
    xf = tok_ref[...].astype(jnp.float32)
    scale = lax.rsqrt(jnp.mean(xf * xf, axis=-1, keepdims=True) + EPS)
    for k in range(n_fs // 2 + 1):
        for ref, s in ((own_ref, sign), (par_ref, -sign)):
            cols = block_cols(z, s, k, n_fs, w)
            part = tok_ref[:, cols].astype(jnp.float32) * scale * gain_ref[:, cols]
            ref[:, k * w : (k + 1) * w] = part.astype(jnp.bfloat16)


def dot1_body(n_x, first, cols, *refs):
    x_refs, w_refs, out_ref = refs[:n_x], refs[n_x:-1], refs[-1]
    w = jnp.concatenate([r[:, cols] for r in w_refs], axis=0)
    span = slice(first, first + w.shape[0])
    for i, x_ref in enumerate(x_refs):
        rows = x_ref.shape[0]
        p = jnp.dot(x_ref[:, span], w, preferred_element_type=jnp.float32)
        out_ref[i * rows : (i + 1) * rows] = p.astype(jnp.bfloat16)


def hidden_body(rows, pa_ref, pb_ref, qa_ref, qb_ref, ha_ref, hb_ref):
    def step(i, _):
        here = pl.ds(pl.multiple_of(i * rows, rows), rows)
        there = pl.ds(pl.multiple_of((i + 1 - 2 * lax.rem(i, 2)) * rows, rows), rows)
        for p_ref, q_ref, h_ref in ((pa_ref, qb_ref, ha_ref), (pb_ref, qa_ref, hb_ref)):
            for j in range(0, p_ref.shape[1], 128):
                cols = slice(j, j + 128)
                pre = p_ref[here, cols].astype(jnp.float32) + q_ref[there, cols].astype(jnp.float32)
                h_ref[here, cols] = jnp.square(jnp.maximum(pre, 0.0)).astype(jnp.bfloat16)
        return 0

    lax.fori_loop(0, pa_ref.shape[0] // rows, step, 0)


def dot2_body(n_x, counts, *refs):
    h_refs, outs = refs[:4], refs[-n_x:]
    w_refs = refs[4:-n_x]
    rows = outs[0].shape[0]
    blocks, pos = [], 0
    for n in counts:
        blocks.append(jnp.concatenate([r[...] for r in w_refs[pos : pos + n]], axis=0))
        pos += n
    runs, col = [], 0
    for w in blocks:
        if runs and runs[-1][0].shape[0] == w.shape[0]:
            runs[-1] = (jnp.concatenate([runs[-1][0], w], axis=1), runs[-1][1])
        else:
            runs.append((w, col))
        col += w.shape[1]
    for w, col in runs:
        n = w.shape[0] // h_refs[0].shape[1]
        for i, o_ref in enumerate(outs):
            h = jnp.concatenate([r[i * rows : (i + 1) * rows] for r in h_refs[:n]], axis=1)
            o = jnp.dot(h, w, preferred_element_type=jnp.float32)
            o_ref[:, col : col + w.shape[1]] = o.astype(jnp.bfloat16)


def sum_body(a_ref, b_ref, c_ref, d_ref, s_ref, u_ref):
    r = a_ref.shape[0] // 2
    tot = a_ref[...].astype(jnp.float32) + b_ref[...].astype(jnp.float32)
    tot = tot + (c_ref[...].astype(jnp.float32) + d_ref[...].astype(jnp.float32))
    s_ref[...] = tot[:r]
    u_ref[...] = tot[r:].astype(jnp.bfloat16)


def final_body(n_fs, groups, tok_ref, *refs):
    z, sign = position()
    n = len(groups)
    s_refs, u_refs, out_ref = refs[:n], refs[n : 2 * n], refs[-1]
    w = tok_ref.shape[1] // n_fs
    half = n_fs // 2
    for s_ref, u_ref, ks in zip(s_refs, u_refs, groups):
        for i, k in enumerate(ks):
            here = slice(i * w, (i + 1) * w)
            s, u = s_ref[:, here], u_ref[:, here].astype(jnp.float32)
            cols = block_cols(z, sign, k, n_fs, w)
            if k in (0, half):
                out_ref[:, cols] = (tok_ref[:, cols].astype(jnp.float32) + (s + u)).astype(jnp.bfloat16)
            else:
                out_ref[:, cols] = (tok_ref[:, cols].astype(jnp.float32) + s).astype(jnp.bfloat16)
                cols = block_cols(z, -sign, k, n_fs, w)
                out_ref[:, cols] = (tok_ref[:, cols].astype(jnp.float32) + u).astype(jnp.bfloat16)


def after(x, *deps):
    return lax.optimization_barrier((x, *deps))[0]


def local(n_fs, n_tp, tokens, norm_gain, w_in, w_out):
    half, n_x = n_fs // 2, n_tp // CORES
    axes = ("fs", "tp")
    every = [(f, t) for f in range(n_fs) for t in range(n_tp)]

    def moved(dest):
        flat = lambda f, t: (f % n_fs) * n_tp + t
        return [(flat(f, t), flat(*dest(f, t))) for f, t in every]

    ring = moved(lambda f, t: (f + 1 - 2 * (t % CORES), t))
    swap = moved(lambda f, t: (f, t ^ 1))
    along = [moved(lambda f, t, d=d: (f, (t + CORES * d) % n_tp)) for d in range(n_x)]
    pz = lambda v: lax.ppermute(v, axes, ring)
    pc = lambda v: lax.ppermute(v, axes, swap)
    px = lambda v, d: lax.ppermute(v, axes, along[d % n_x])

    rows, d_model = tokens.shape
    width = d_model // n_fs
    f_own = w_in.shape[1]

    shape = jax.ShapeDtypeStruct((rows, (half + 1) * width), jnp.bfloat16)
    own, par = call(
        functools.partial(norm_body, n_fs),
        "norm",
        (shape, shape),
        (tokens, norm_gain.astype(jnp.float32).reshape(1, d_model)),
        rows * d_model * 8,
    )
    chip = jnp.concatenate([own, pc(par)], axis=0)

    def halves(v):
        h = v.shape[0] // 2
        return [v[:h], v[h:]]

    in_a, in_b = [halves(w_in)], [[pc(v) for v in halves(w_in)]]
    out_a, out_b = [halves(w_out)], [[pc(v) for v in halves(w_out)]]

    def ring_step(chain, *deps):
        chain.append([pz(after(v, *deps)) for v in chain[-1]])

    last = ()
    for k in range(1, half + 1):
        turn = out_a if k % 2 else out_b
        ring_step(turn, in_a[-1][0])
        ring_step(in_a, *last)
        if k < half:
            ring_step(in_b, *last)
        last = turn[-1]

    chunks = [chip] + [px(chip, d) for d in range(1, n_x)]
    a_all = [v for blk in in_a for v in blk]
    b_all = [v for blk in in_b[1:half] for v in blk]
    total = n_x * CORES * rows
    piece = jax.ShapeDtypeStruct((total, f_own // 2), jnp.bfloat16)
    hidden = [None] * 4
    for j in range(2):
        cols = slice(j * piece.shape[1], (j + 1) * piece.shape[1])
        parts = [
            call(
                functools.partial(dot1_body, n_x, first, cols),
                "dot1",
                piece,
                (*chunks, *w),
                2 * total * len(w) * w[0].shape[0] * piece.shape[1],
            )
            for first, w in ((0, a_all), (width, b_all))
        ]
        hidden[j], hidden[2 + j] = call(
            functools.partial(hidden_body, rows),
            "hidden",
            (piece, piece),
            (*parts, *[pc(p) for p in parts]),
            piece.size * 400,
        )

    def group_parts(ks):
        blocks, counts = [], []
        for k in ks:
            blk = out_a[k] + (out_b[k] if 0 < k < half else [])
            blocks += blk
            counts.append(len(blk))
        o_shape = jax.ShapeDtypeStruct((CORES * rows, len(ks) * width), jnp.bfloat16)
        parts = call(
            functools.partial(dot2_body, n_x, tuple(counts)),
            "dot2",
            (o_shape,) * n_x,
            (*hidden, *blocks),
            2 * n_x * CORES * rows * CORES * f_own * len(ks) * width,
        )
        return parts, [parts[0]] + [px(parts[d], -d) for d in range(1, n_x)]

    def group_sum(got):
        r, c = got[0].shape
        s, u = call(
            sum_body,
            "sum",
            (jax.ShapeDtypeStruct((rows, c), jnp.float32), jax.ShapeDtypeStruct((rows, c), jnp.bfloat16)),
            got,
            4 * r * c,
        )
        return s, pc(u)

    groups = [(0, 1, 2, 3), (4, 5, 6), tuple(range(7, half + 1))]
    ring_step(out_a)
    ring_step(out_b)
    ring_step(out_a, *hidden)
    ring_step(out_b, *hidden)
    parts, first = group_parts(groups[0])
    ring_step(out_a, parts[0])
    ring_step(out_b, parts[0])
    parts, second = group_parts(groups[1])
    ring_step(out_a, parts[0])
    _, third = group_parts(groups[2])
    done = [group_sum(g) for g in (first, second, third)]
    sums, sides = zip(*done)
    return call(
        functools.partial(final_body, n_fs, groups),
        "final",
        jax.ShapeDtypeStruct(tokens.shape, jnp.bfloat16),
        (tokens, *sums, *sides),
        rows * d_model * 4,
    )


def solution(mesh):
    in_specs = (P(("grp", "fs", "tp"), None), P(), P("fs", "tp"), P("tp", "fs"))
    out_specs = P(("grp", "fs", "tp"), None)
    body = functools.partial(local, mesh.shape["fs"], mesh.shape["tp"])
    return jax.shard_map(body, mesh=mesh, in_specs=in_specs, out_specs=out_specs, check_vma=False)
```
